32 devices in a mesh: sp: 8 (over z, x), tp: 4 (over y, core).
Axes of the slice: x: 2, y: 2, z: 4, core: 2. Of those that a mesh axis runs over, the one named last changes fastest.
Arguments:
- residual: bfloat16 [1024, 2048], P('sp', 'tp'), may hold values from -80 to 80
- query_wide: bfloat16 [1024, 1024], P('sp', 'tp'), may hold values from -6 to 6
- key_wide: bfloat16 [1024, 1024], P('sp', 'tp'), may hold values from -6 to 6
- query_narrow: bfloat16 [1024, 512], P('sp', 'tp'), may hold values from -6 to 6
- key_narrow: bfloat16 [1024, 512], P('sp', 'tp'), may hold values from -6 to 6
- values: bfloat16 [1024, 2048], P('sp', 'tp'), may hold values from -6 to 6
- gate_logits: float32 [4, 8, 1024], P(None, 'tp', 'sp'), may hold values from -6 to 106
- head_gain: float32 [2048], P('tp'), may hold values from 0.1 to 1.9
- norm_gain: float32 [2048], replicated, may hold values from 0.1 to 1.9
- route_experts: int32 [1024, 2], P('sp'), may hold values from 0 to 7, all different within a row; in each aligned block of 128 rows (0 to 127, 128 to 255, ...) at most 64 rows name the same one
- route_weights: float32 [1024, 2], P('sp'), may hold values from 0.2 to 1
- expert_gate: bfloat16 [8, 2048, 3584], P('sp', None, 'tp'), may hold values from -0.125 to 0.125
- expert_up: bfloat16 [8, 2048, 3584], P('sp', None, 'tp'), may hold values from -0.125 to 0.125
- expert_down: bfloat16 [8, 3584, 2048], P('sp', 'tp'), may hold values from -0.09375 to 0.09375
Outputs:
- layer_out: bfloat16 [1024, 2048], P('sp', 'tp')
The draws below stay inside these ranges and needn't reach their ends.
Inputs may be any that keep to these rules, and one draw needn't show every extreme that they name: `route_experts`: each row names 2 different experts; within the rows of one device (aligned blocks of 128 rows) no expert is named more than 64 times, a bound that some block reaches.
All inputs are finite; a program needn't handle non-finite values.
Results may differ from the reference program's by a relative error of at most 0.0055.
Values may be sent and summed in bfloat16 or wider, within the bound.
A program may use at most 128 MiB of HBM per device.

```python
import math
import jax
import jax.numpy as jnp
import numpy as np
from jax import lax

HEADS = 4
DKW = 256
DKN = 128
DV = 256
FF = 3584
TOP = 2
BLOCK = 64
TOK_DEV = 128
D = 2048
TOKENS = 1024
EXPERTS = 8
CAP = 64
N_SP = 8
N_TP = 4


def draw_residual(key, part):
    first, second = jax.random.split(key, 2)
    column_log = jax.random.uniform(second, (16,), jnp.float32, -1.2, 1.2)
    column_scale = jnp.exp(jnp.repeat(column_log, D // 16))
    noise = jnp.clip(jax.random.normal(first, (TOKENS, D), jnp.float32), -6.0, 6.0)
    return (noise * column_scale[None, :]).astype(jnp.bfloat16)


def draw_gate_logits(key, part):
    subkeys = jax.random.split(key, 3)
    head_total = 2 * HEADS
    noise = jnp.clip(jax.random.normal(subkeys[0], (4, head_total, TOKENS), jnp.float32), -4.0, 4.0)
    span_count = TOKENS // TOK_DEV
    block_shift = jax.random.uniform(subkeys[1], (4, head_total, span_count), jnp.float32, -0.9, 0.9)
    block_shift = jnp.repeat(block_shift, TOK_DEV, axis=2)
    ranking = jnp.stack([jax.random.permutation(jax.random.fold_in(subkeys[2], side), head_total) for side in range(2)])
    quick = (ranking < head_total // 2).astype(jnp.float32)
    keep_base = 11.5 - 8.0 * quick
    forget = keep_base[:, :, None] + 0.7 * noise[1::2] + block_shift[1::2]
    incoming = 1.2 * noise[0::2] + block_shift[0::2]
    return jnp.stack([incoming[0], forget[0], incoming[1], forget[1]])


def level_of(rng, dims, pieces, least, top_value):
    gain = 1.0
    for axis_at, shards_of in pieces:
        draws = jax.random.uniform(jax.random.fold_in(jax.random.fold_in(rng, 6), axis_at), (shards_of,), jnp.float32, least / len(pieces), top_value / len(pieces))
        gain = gain * jnp.repeat(jnp.exp(draws), dims[axis_at] // shards_of).reshape((-1,) + (1,) * (len(dims) - 1 - axis_at))
    return gain


def shared_out(rng, own, number, rows, amount, top, reach, skew):
    sequence = jax.random.permutation(rng, amount)
    heavy_load, usual = shares(amount, rows * top, reach, skew, True), shares(amount, rows * top, reach, skew, False)
    places = jnp.arange(amount)

    def named(tallies, offset_by):
        used = int((tallies > 0).sum())
        fixed = max(1, used // 4)
        moved = fixed + (places - fixed + offset_by * (used - fixed)) % max(1, amount - fixed)
        return jnp.zeros((amount,), jnp.int32).at[sequence[jnp.where(places < fixed, places, moved)]].set(jnp.asarray(tallies, jnp.int32))

    tallies = jnp.where(number % 4 == 0, named(heavy_load, number // 4), named(usual, number - number // 4 - 1))
    mixed = jax.random.permutation(jax.random.fold_in(own, 3), amount)
    source_of, taker = mixed[0:amount // 2 * 2:2], mixed[1:amount // 2 * 2:2]
    slack = jnp.minimum(tallies[source_of] - 1, reach - tallies[taker]) // 2
    slack = jnp.where((source_of == sequence[0]) | (taker == sequence[0]) | (tallies[taker] == 0), 0, jnp.maximum(slack, 0))
    moved = jax.random.randint(jax.random.fold_in(own, 4), (amount // 2,), 0, 1 << 20) % (slack + 1)
    tallies = tallies.at[source_of].add(-moved).at[taker].add(moved)
    labels = jnp.searchsorted(jnp.cumsum(tallies), jnp.arange(rows * top), side="right").astype(jnp.int32)
    table = labels.reshape(top, rows).T
    table = table[jax.random.permutation(jax.random.fold_in(own, 1), rows)]
    offset_by = jax.random.randint(jax.random.fold_in(own, 2), (rows, 1), 0, top)
    return jnp.take_along_axis(table, (jnp.arange(top)[None, :] + offset_by) % top, axis=1)


def shares(number_of, total, bound, slope, full):
    weights = [(1 << 20) // math.isqrt(rank ** slope) + 1 for rank in range(1, number_of + 1)]
    largest = bound if full else min(bound, max(-(-total // number_of), total * weights[0] // sum(weights)))
    least = 1 if total - largest >= number_of - 1 else 0
    holding, spare = [largest] + [least] * (number_of - 1), total - largest - least * (number_of - 1)
    while spare > 0:
        candidates = [i for i in range(1, number_of) if holding[i] < largest] or [i for i in range(1, number_of) if holding[i] < bound]
        pool, budget = sum([weights[i] for i in candidates]), spare
        for i in candidates:
            extra = min(bound - holding[i], max(1, budget * weights[i] // pool), spare)
            holding[i] = holding[i] + extra
            spare = spare - extra
    return np.array(holding)


def gaussian(key, extent, width, limit, cuts=(), held_as=jnp.bfloat16):
    entries = jax.random.normal(key, extent, jnp.float32) * width
    if len(cuts) > 0:
        entries = level_of(key, extent, cuts, -0.22, 0.18) * entries
    return jnp.clip(entries, min=-limit, max=limit).astype(held_as)


def setup_inputs(seed: int = 0) -> dict:
    arg_keys = jax.random.split(jax.random.key(seed), 15)
    residual = draw_residual(jax.random.fold_in(arg_keys[14], 71), 0)
    query_wide = gaussian(arg_keys[1], (TOKENS, HEADS * DKW), 1.0, 6.0, ((0, 8), (1, 4)))
    key_wide = gaussian(arg_keys[2], (TOKENS, HEADS * DKW), 1.0, 6.0, ((0, 8), (1, 4)))
    query_narrow = gaussian(arg_keys[3], (TOKENS, HEADS * DKN), 1.0, 6.0, ((0, 8), (1, 4)))
    key_narrow = gaussian(arg_keys[4], (TOKENS, HEADS * DKN), 1.0, 6.0, ((0, 8), (1, 4)))
    values = gaussian(arg_keys[5], (TOKENS, D), 1.0, 6.0, ((0, 8), (1, 4)))
    gate_logits = draw_gate_logits(jax.random.fold_in(arg_keys[14], 71), 0)
    head_gain = jnp.clip(1.0 + 0.18 * jax.random.normal(arg_keys[7], (D,), jnp.float32), 0.1, 1.9)
    norm_gain = jnp.clip(1.0 + 0.18 * jax.random.normal(arg_keys[8], (D,), jnp.float32), 0.1, 1.9)
    route_experts_keys = jax.random.split(jax.random.fold_in(arg_keys[9], 1), TOKENS // TOK_DEV)
    route_experts_turns = jax.random.permutation(jax.random.fold_in(arg_keys[9], 3), TOKENS // TOK_DEV)
    route_experts = jax.vmap(lambda own, number: shared_out(jax.random.fold_in(arg_keys[9], 2), own, number, TOK_DEV, EXPERTS, TOP, CAP, 1))(route_experts_keys, route_experts_turns).reshape((TOKENS, TOP))
    route_weights = jnp.clip(0.2 + 0.8 * jax.random.uniform(arg_keys[10], (TOKENS, TOP), jnp.float32) ** level_of(arg_keys[10], (TOKENS, TOP), ((0, 8),), -0.2, 0.2), 0.2, 1.0)
    expert_gate = gaussian(arg_keys[11], (EXPERTS, D, FF), D ** -0.5, 0.125, ((0, 8), (2, 4)))
    expert_up = gaussian(arg_keys[12], (EXPERTS, D, FF), D ** -0.5, 0.125, ((0, 8), (2, 4)))
    expert_down = gaussian(arg_keys[13], (EXPERTS, FF, D), FF ** -0.5, 0.09375, ((0, 8), (1, 4)))
    return {"residual": residual, "query_wide": query_wide, "key_wide": key_wide, "query_narrow": query_narrow, "key_narrow": key_narrow, "values": values, "gate_logits": gate_logits, "head_gain": head_gain, "norm_gain": norm_gain, "route_experts": route_experts, "route_weights": route_weights, "expert_gate": expert_gate, "expert_up": expert_up, "expert_down": expert_down}


precise = lax.Precision.HIGHEST
norm_eps = 1e-06

def blockwise(query_heads, key_heads, value_heads, log_in, log_keep):
    head_count, length, key_width = query_heads.shape
    value_width = value_heads.shape[-1]
    block_count = length // BLOCK

    def to_blocks(array):
        return jnp.moveaxis(array.reshape((head_count, block_count, BLOCK) + array.shape[2:]), 1, 0)
    inputs = (to_blocks(query_heads), to_blocks(key_heads), to_blocks(value_heads), to_blocks(log_in), to_blocks(log_keep))
    lower_mask = jnp.tril(jnp.ones((BLOCK, BLOCK), dtype=bool))

    def advance(carried, block_in):
        memory, normer, stabilizer = carried
        query_b, key_b, value_b, in_b, keep_b = block_in
        running = jnp.cumsum(keep_b, axis=-1)
        log_weights = jnp.where(lower_mask[None], running[:, :, None] - running[:, None, :] + in_b[:, None, :], -jnp.inf)
        carry_log = running + stabilizer[:, None]
        highest = jnp.maximum(carry_log, lax.optimization_barrier(jnp.max(log_weights, axis=-1)))
        carry_w = jnp.exp(carry_log - highest)
        scores = jnp.einsum('hld,hsd->hls', query_b, key_b, precision=precise)
        intra_w = jnp.exp(log_weights - highest[:, :, None]) * scores
        numerator = carry_w[..., None] * jnp.einsum('hld,hde->hle', query_b, memory, precision=precise) + jnp.einsum('hls,hse->hle', intra_w, value_b, precision=precise)
        divisor = carry_w * jnp.einsum('hld,hd->hl', query_b, normer, precision=precise) + lax.optimization_barrier(jnp.sum(intra_w, axis=-1))
        output = numerator / jnp.maximum(jnp.abs(divisor), jnp.exp(-highest))[..., None]
        total_log = running[:, -1]
        later_log = total_log[:, None] - running + in_b
        new_stab = jnp.maximum(total_log + stabilizer, lax.optimization_barrier(jnp.max(later_log, axis=-1)))
        decay_old = jnp.exp(total_log + stabilizer - new_stab)
        weighted = key_b * jnp.exp(later_log - new_stab[:, None])[..., None]
        memory = decay_old[:, None, None] * memory + jnp.einsum('hsd,hse->hde', weighted, value_b, precision=precise)
        normer = decay_old[:, None] * normer + lax.optimization_barrier(jnp.sum(weighted, axis=1))
        return ((memory, normer, new_stab), output)
    start = (jnp.zeros((head_count, key_width, value_width), jnp.float32), jnp.zeros((head_count, key_width), jnp.float32), jnp.full((head_count,), -jnp.inf, jnp.float32))
    _, results = lax.scan(advance, start, inputs)
    return jnp.moveaxis(results, 0, 1).reshape(head_count, length, value_width)

def reverse_seq(array):
    return jnp.flip(array, axis=1)

def reference(residual, query_wide, key_wide, query_narrow, key_narrow, values, gate_logits, head_gain, norm_gain, route_experts, route_weights, expert_gate, expert_up, expert_down):
    value_all = values.astype(jnp.float32).reshape(TOKENS, HEADS, 2, DV)
    results = []
    for group_index, (query_in, key_in, key_width) in enumerate(((query_wide, key_wide, DKW), (query_narrow, key_narrow, DKN))):
        query_heads = query_in.astype(jnp.float32).reshape(TOKENS, HEADS, key_width).transpose(1, 0, 2)
        key_heads = key_in.astype(jnp.float32).reshape(TOKENS, HEADS, key_width).transpose(1, 0, 2) * key_width ** (-0.5)
        value_heads = value_all[:, :, group_index].transpose(1, 0, 2)
        gates_here = gate_logits[:, group_index::2]
        forward = blockwise(query_heads, key_heads, value_heads, gates_here[0], jax.nn.log_sigmoid(gates_here[1]))
        backward = reverse_seq(blockwise(reverse_seq(query_heads), reverse_seq(key_heads), reverse_seq(value_heads), reverse_seq(gates_here[2]), reverse_seq(jax.nn.log_sigmoid(gates_here[3]))))
        results.append(forward + backward)
    stacked = jnp.stack(results, axis=1)
    stacked = stacked * lax.rsqrt(lax.optimization_barrier(jnp.mean(stacked * stacked, axis=-1, keepdims=True)) + norm_eps)
    stacked = stacked * head_gain.reshape(HEADS, 2, 1, DV)
    heads_out = stacked.transpose(2, 0, 1, 3).reshape(TOKENS, D)
    merged = (residual.astype(jnp.float32) + heads_out).astype(jnp.bfloat16)
    merged_f = merged.astype(jnp.float32)
    normed = (merged_f * lax.rsqrt(lax.optimization_barrier(jnp.mean(merged_f * merged_f, axis=-1, keepdims=True)) + norm_eps) * norm_gain).astype(jnp.bfloat16)
    capacity = N_SP * CAP
    quarter = FF // N_TP

    def expert_step(expert, accumulated):
        chosen = route_experts == expert
        weight_row = lax.optimization_barrier(jnp.sum(jnp.where(chosen, route_weights, 0.0), axis=1))
        taken = jnp.any(chosen, axis=1)
        row_index = jnp.nonzero(taken, size=capacity, fill_value=0)[0].astype(jnp.int32)
        occupied = jnp.arange(capacity) < jnp.sum(taken.astype(jnp.int32))
        features = normed[row_index]
        gate_proj = jnp.dot(features, expert_gate[expert], preferred_element_type=jnp.float32)
        up_proj = jnp.dot(features, expert_up[expert], preferred_element_type=jnp.float32)
        hidden = (jax.nn.silu(gate_proj) * up_proj).astype(jnp.bfloat16)
        summed = jnp.zeros((capacity, D), jnp.float32)
        for block_index in range(N_TP):
            partial_sum = jnp.dot(hidden[:, block_index * quarter:(block_index + 1) * quarter], expert_down[expert, block_index * quarter:(block_index + 1) * quarter], preferred_element_type=jnp.float32)
            summed = summed + lax.optimization_barrier(partial_sum.astype(jnp.bfloat16)).astype(jnp.float32)
        result = lax.optimization_barrier(summed.astype(jnp.bfloat16)).astype(jnp.float32)
        mix_weight = jnp.where(occupied, weight_row[row_index], 0.0)
        return accumulated.at[row_index].add(result * mix_weight[:, None])
    added = lax.fori_loop(0, EXPERTS, expert_step, jnp.zeros((TOKENS, D), jnp.float32))
    return (merged_f + added).astype(jnp.bfloat16)
```

```python
import functools

import jax
import jax.numpy as jnp
from jax import lax
from jax.experimental import pallas as pl
from jax.experimental.pallas import tpu as pltpu
from jax.sharding import PartitionSpec as P

precise = lax.Precision.HIGHEST
norm_eps = 1e-06


def prefix(part, axis, combine, identity, reverse):
    count = lax.axis_size(axis)
    place = lax.axis_index(axis)
    ahead = count - 1 - place if reverse else place
    gathered = jax.tree.map(lambda a: lax.all_gather(a, axis), part)
    state = jax.tree.map(lambda a, e: jnp.zeros_like(a) + jnp.asarray(e, a.dtype), part, identity)

    def one(step, state):
        source = count - 1 - step if reverse else step
        return combine(
            state, jax.tree.map(lambda a: lax.dynamic_index_in_dim(a, source, 0, False), gathered)
        )

    return lax.fori_loop(0, ahead, one, state)


def summarize(inputs):
    query_heads, key_heads, value_heads, log_in, log_keep = inputs
    running = jnp.cumsum(log_keep, axis=-1)
    total_log = running[:, -1]
    later_log = total_log[:, None] - running + log_in
    highest = jnp.max(later_log, axis=-1)
    weighted = key_heads * jnp.exp(later_log - highest[:, None])[..., None]
    memory = jnp.einsum("hsd,hse->hde", weighted, value_heads, precision=precise)
    return (memory, jnp.sum(weighted, axis=1), highest, total_log)


def empty_state(template):
    memory, normer, stabilizer, total_log = template
    return (
        jnp.zeros_like(memory),
        jnp.zeros_like(normer),
        jnp.full_like(stabilizer, -1e30),
        jnp.zeros_like(total_log),
    )


def join_states(earlier, later):
    joined = []
    for offset in range(0, len(earlier), 4):
        mem_old, norm_old, stab_old, total_old = earlier[offset : offset + 4]
        mem_new, norm_new, stab_new, total_new = later[offset : offset + 4]
        highest = jnp.maximum(stab_old + total_new, stab_new)
        old_scale = jnp.exp(stab_old + total_new - highest)
        new_scale = jnp.exp(stab_new - highest)
        joined += [
            old_scale[:, None, None] * mem_old + new_scale[:, None, None] * mem_new,
            old_scale[:, None] * norm_old + new_scale[:, None] * norm_new,
            highest,
            total_old + total_new,
        ]
    return tuple(joined)


def log_table(inputs):
    query_heads, key_heads, value_heads, log_in, log_keep = inputs
    running = jnp.cumsum(log_keep, axis=-1)
    positions = jnp.arange(running.shape[1])
    lower_mask = positions[:, None] >= positions[None, :]
    log_weights = jnp.where(
        lower_mask[None], running[:, :, None] - running[:, None, :] + log_in[:, None, :], -jnp.inf
    )
    scores = jnp.einsum("hld,hsd->hls", query_heads, key_heads, precision=precise)
    return (running, log_weights, scores)


def full_pass(inputs, carried):
    query_heads, value_heads = (inputs[0], inputs[2])
    memory, normer, stabilizer, total_log = carried
    running, log_weights, scores = log_table(inputs)
    carry_log = running + stabilizer[:, None]
    highest = jnp.maximum(carry_log, jnp.max(log_weights, axis=-1))
    carry_w = jnp.exp(carry_log - highest)
    intra_w = jnp.exp(log_weights - highest[:, :, None]) * scores
    numerator = carry_w[..., None] * jnp.einsum(
        "hld,hde->hle", query_heads, memory, precision=precise
    )
    numerator = numerator + jnp.einsum("hls,hse->hle", intra_w, value_heads, precision=precise)
    divisor = carry_w * jnp.einsum("hld,hd->hl", query_heads, normer, precision=precise) + jnp.sum(
        intra_w, axis=-1
    )
    return numerator / jnp.maximum(jnp.abs(divisor), jnp.exp(-highest))[..., None]


def body(
    residual,
    query_wide,
    key_wide,
    query_narrow,
    key_narrow,
    values,
    gate_logits,
    head_gain,
    norm_gain,
    route_experts,
    route_weights,
    expert_gate,
    expert_up,
    expert_down,
):
    heads_here = gate_logits.shape[1] // 2
    tok_rows = residual.shape[0]
    value_width = values.shape[1] // (2 * heads_here)
    value_all = values.astype(jnp.float32).reshape(tok_rows, heads_here, 2, value_width)
    groups = []
    for group_index, (query_in, key_in) in enumerate(
        ((query_wide, key_wide), (query_narrow, key_narrow))
    ):
        key_width = query_in.shape[1] // heads_here
        query_heads = (
            query_in.astype(jnp.float32).reshape(tok_rows, heads_here, key_width).transpose(1, 0, 2)
        )
        key_heads = key_in.astype(jnp.float32).reshape(tok_rows, heads_here, key_width).transpose(
            1, 0, 2
        ) * key_width ** (-0.5)
        value_heads = value_all[:, :, group_index].transpose(1, 0, 2)
        gates_here = gate_logits[:, group_index::2]
        ahead = (
            query_heads,
            key_heads,
            value_heads,
            gates_here[0],
            jax.nn.log_sigmoid(gates_here[1]),
        )
        behind = tuple(
            (
                jnp.flip(array, axis=1)
                for array in (
                    query_heads,
                    key_heads,
                    value_heads,
                    gates_here[2],
                    jax.nn.log_sigmoid(gates_here[3]),
                )
            )
        )
        groups.append((ahead, behind))
    forward_local = summarize(groups[0][0]) + summarize(groups[1][0])
    backward_local = summarize(groups[0][1]) + summarize(groups[1][1])
    forward_in = prefix(
        forward_local,
        "sp",
        join_states,
        empty_state(forward_local[:4]) + empty_state(forward_local[4:]),
        False,
    )
    backward_in = prefix(
        backward_local,
        "sp",
        join_states,
        empty_state(backward_local[:4]) + empty_state(backward_local[4:]),
        True,
    )
    cells = []
    for group_index, pair in enumerate(groups):
        halves = []
        for side, inputs in enumerate(pair):
            carried = (forward_in, backward_in)[side][4 * group_index : 4 * group_index + 4]
            output = full_pass(inputs, carried)
            if side == 1:
                output = jnp.flip(output, axis=1)
            halves.append(output)
        cells.append(halves[0] + halves[1])
    stacked = jnp.stack(cells, axis=1)
    stacked = stacked * lax.rsqrt(jnp.mean(stacked * stacked, axis=-1, keepdims=True) + norm_eps)
    stacked = stacked * head_gain.reshape(heads_here, 2, 1, value_width)
    heads_out = stacked.transpose(2, 0, 1, 3).reshape(tok_rows, -1)
    merged = (residual.astype(jnp.float32) + heads_out).astype(jnp.bfloat16)
    merged_f = merged.astype(jnp.float32)
    expert_total = lax.axis_size("sp")
    top_count = route_experts.shape[1]
    capacity = 2 * top_count * tok_rows // expert_total
    picks = route_experts.reshape(-1)
    pick_count = picks.shape[0]
    onehot = (picks[:, None] == jnp.arange(expert_total, dtype=jnp.int32)[None, :]).astype(
        jnp.int32
    )
    before = jnp.cumsum(onehot, axis=0) - onehot
    ranking = jnp.sum(before * onehot, axis=1)
    slot_of = picks * capacity + ranking
    owner = jnp.arange(pick_count, dtype=jnp.int32) // top_count
    source_row = jnp.zeros((expert_total * capacity,), jnp.int32).at[slot_of].set(owner)
    filled = jnp.zeros((expert_total * capacity,), jnp.bool_).at[slot_of].set(True)
    squares = lax.psum(jnp.sum(merged_f * merged_f, axis=1), "tp")
    own_width = merged.shape[1]
    gain_part = lax.dynamic_slice_in_dim(norm_gain, lax.axis_index("tp") * own_width, own_width)
    scale_row = lax.rsqrt(squares / (own_width * lax.axis_size("tp")) + norm_eps)
    normed = (merged_f * scale_row[:, None] * gain_part).astype(jnp.bfloat16)
    zero_row = jnp.zeros((), jnp.bfloat16)
    gathered = lax.all_gather(
        lax.all_to_all(
            jnp.where(filled[:, None], normed[source_row], zero_row).reshape(
                expert_total, capacity, -1
            ),
            "sp",
            split_axis=0,
            concat_axis=0,
            tiled=True,
        ),
        "tp",
        axis=2,
        tiled=True,
    )
    sources, slots, width_all = gathered.shape
    flat_rows = gathered.reshape(sources * slots, width_all)
    gate_proj = jnp.dot(flat_rows, expert_gate[0], preferred_element_type=jnp.float32)
    up_proj = jnp.dot(flat_rows, expert_up[0], preferred_element_type=jnp.float32)
    hidden = (jax.nn.silu(gate_proj) * up_proj).astype(jnp.bfloat16)
    partial_value = jnp.dot(hidden, expert_down[0], preferred_element_type=jnp.float32)
    summed = lax.psum_scatter(
        partial_value.astype(jnp.bfloat16), "tp", scatter_dimension=1, tiled=True
    )
    back = summed.reshape(sources, slots, -1)
    returned = lax.all_to_all(back, "sp", split_axis=0, concat_axis=0, tiled=True)
    flat_back = returned.reshape(expert_total * capacity, -1).astype(jnp.float32)
    picked = flat_back[slot_of] * route_weights.reshape(-1)[:, None]
    added = jnp.sum(picked.reshape(tok_rows, top_count, -1), axis=1)
    return (merged_f + added).astype(jnp.bfloat16)


MESH = pl.DeviceIdType.MESH
FAR = -1e30


def log_sigmoid(x):
    return jnp.minimum(x, 0.0) - jnp.log1p(jnp.exp(-jnp.abs(x)))


def layer_kernel(
    n,
    groups,
    pieces,
    heads_here,
    *refs,
):
    small_count = 11
    sources = refs[:small_count]
    gate_hbm, up_hbm, down_hbm, out = refs[small_count : small_count + 4]
    held = refs[small_count + 4 : 2 * small_count + 4]
    (
        residual,
        query_wide,
        key_wide,
        query_narrow,
        key_narrow,
        values,
        gates,
        head_gain,
        norm_gain,
        route_experts,
        route_weights,
    ) = held
    (
        gates_all,
        key_wide_all,
        key_narrow_all,
        values_all,
        col_weight,
        acc,
        den,
        slots_out,
        rows_in,
        lhs,
        hidden,
        partial_out,
        sib_in,
        pair_sum,
        cross_in,
        final,
        back,
        gate_w,
        up_w,
        down_w,
        out_held,
        weight_sem,
        small_sem,
        out_sem,
        gate_send,
        gate_recv,
        kv_send,
        kv_recv,
        row_send,
        row_recv,
        sib_send,
        sib_recv,
        cross_send,
        cross_recv,
        back_send,
        back_recv,
    ) = refs[2 * small_count + 4 :]
    me = lax.axis_index("sp")
    col = lax.axis_index("tp")
    n_tp = lax.axis_size("tp")
    stations = n // 2
    station = me // 2
    side = me % 2
    pair = station * 2 + (1 - side)
    sib = (col // 2) * 2 + (1 - col % 2)
    cross = (col + 2) % n_tp
    cross_sib = (sib + 2) % n_tp
    rows, width = residual.shape
    cap = slots_out.shape[1]
    per_group = n // groups
    group_rows = per_group * cap
    head_count = 2 * heads_here
    dv = width // head_count

    barrier = pltpu.get_barrier_semaphore()
    for k in range(1, n):
        pl.semaphore_signal(
            barrier, inc=1, device_id=((me + k) % n, col), device_id_type=MESH
        )
    for k in range(1, n_tp):
        pl.semaphore_signal(
            barrier, inc=1, device_id=(me, (col + k) % n_tp), device_id_type=MESH
        )
    load = [
        pltpu.make_async_copy(src, dst, small_sem.at[i])
        for i, (src, dst) in enumerate(zip(sources, held))
    ]
    for i in (6, 2, 4, 5, 1, 3, 0, 7, 8, 9, 10):
        load[i].start()
    fetch = [
        pltpu.make_async_copy(src.at[0], dst, weight_sem.at[i])
        for i, (src, dst) in enumerate(((gate_hbm, gate_w), (up_hbm, up_w), (down_hbm, down_w)))
    ]
    for copy in fetch:
        copy.start()

    for copy in load:
        copy.wait()
    pl.semaphore_wait(barrier, n - 1 + n_tp - 1)

    def remote(src, dst, send, recv, sp, tp):
        return pltpu.make_async_remote_copy(
            src_ref=src,
            dst_ref=dst,
            send_sem=send,
            recv_sem=recv,
            device_id=(sp, tp),
            device_id_type=MESH,
        )

    def gate_copy(k, source):
        return remote(
            gates,
            gates_all.at[source],
            gate_send.at[k],
            gate_recv.at[source],
            (me + k) % n,
            col,
        )

    for k in range(1, n):
        gate_copy(k, me).start()

    streams = ((key_wide, key_wide_all), (key_narrow, key_narrow_all), (values, values_all))

    def kv_copies(kind, block, own, target):
        return [
            remote(
                local if own else whole.at[block],
                whole.at[block],
                kv_send.at[kind, a, block],
                kv_recv.at[a, block],
                target,
                col,
            )
            for a, (local, whole) in enumerate(streams)
        ]

    def each(copies, act):
        for copy in copies:
            getattr(copy, act)()

    up_there = station < stations - 1
    down_there = station > 0

    @pl.when(up_there)
    def _():
        each(kv_copies(1, me, True, me + 2), "start")

    @pl.when(down_there)
    def _():
        each(kv_copies(2, me, True, me - 2), "start")

    each(kv_copies(0, me, True, pair), "start")

    gates_all[me] = gates[...]
    for k in range(1, n):
        gate_copy(k, (me - k + n) % n).wait_recv()

    t_iota = lax.broadcasted_iota(jnp.int32, (rows, rows), 0)
    s_iota = lax.broadcasted_iota(jnp.int32, (rows, rows), 1)
    lower = (t_iota >= s_iota).astype(jnp.float32)
    upper = (t_iota <= s_iota).astype(jnp.float32)
    strict_low = (t_iota > s_iota).astype(jnp.float32)
    strict_up = (t_iota < s_iota).astype(jnp.float32)
    exact = functools.partial(
        jnp.dot, precision=precise, preferred_element_type=jnp.float32
    )
    n_iota = lax.broadcasted_iota(jnp.int32, (n, rows), 0)

    queries = []
    for h in range(head_count):
        j, g = h // 2, h % 2
        q_ref, k_ref, k_all = (
            (query_wide, key_wide, key_wide_all),
            (query_narrow, key_narrow, key_narrow_all),
        )[g]
        dk = q_ref.shape[1] // heads_here
        queries.append((q_ref, k_ref, k_all, j * dk, dk))

    def scores_of(h, keys):
        q_ref, _, _, start, dk = queries[h]
        return lax.dot_general(
            q_ref[:, start : start + dk],
            keys,
            (((1,), (1,)), ((), ())),
            preferred_element_type=jnp.float32,
        ) * (dk ** (-0.5))

    def weighted_values(weights, vals):
        high = weights.astype(jnp.bfloat16)
        low = (weights - high.astype(jnp.float32)).astype(jnp.bfloat16)
        return jnp.dot(high, vals, preferred_element_type=jnp.float32) + jnp.dot(
            low, vals, preferred_element_type=jnp.float32
        )

    def row_of(plane, h):
        return plane * head_count + h

    own_parts = []
    for h in range(head_count):
        own_scores = scores_of(
            h, queries[h][1][:, queries[h][3] : queries[h][3] + queries[h][4]]
        )
        own_values = values[:, h * dv : (h + 1) * dv]
        halves = []
        for d in range(2):
            keep = log_sigmoid(gates_all[:, row_of(2 * d + 1, h), :])
            log_in = gates_all[:, row_of(2 * d, h), :]
            later = exact(keep, strict_low if d == 0 else strict_up) + log_in
            totals = jnp.sum(keep, axis=1, keepdims=True)
            between = jnp.zeros((n, rows), jnp.float32)
            for i in range(n):
                if d == 0:
                    inside = (n_iota < i) & (i < me)
                else:
                    inside = (n_iota > i) & (i > me)
                between = between + jnp.where(inside, totals[i : i + 1, :], 0.0)
            beyond = (n_iota < me) if d == 0 else (n_iota > me)
            later = jnp.where(beyond, later + between, FAR)
            top = jnp.max(jnp.max(later, axis=1, keepdims=True), axis=0, keepdims=True)
            col_weight[d, h] = jnp.where(beyond, jnp.exp(later - top), 0.0)
            keep_row = log_sigmoid(gates[row_of(2 * d + 1, h) : row_of(2 * d + 1, h) + 1, :])
            in_row = gates[row_of(2 * d, h) : row_of(2 * d, h) + 1, :]
            mask = lower if d == 0 else upper
            run_col = jnp.sum(mask * keep_row, axis=1, keepdims=True)
            keep_rows = jnp.broadcast_to(keep_row, (8, rows))
            run_row = exact(keep_rows, upper if d == 0 else lower)[0:1, :]
            logs = jnp.where(mask > 0.5, run_col - run_row + in_row, FAR)
            highest = jnp.maximum(jnp.max(logs, axis=1, keepdims=True), run_col + top)
            carry = jnp.exp(run_col + top - highest)
            weights = jnp.exp(logs - highest) * own_scores
            halves.append(
                (
                    weighted_values(weights, own_values),
                    jnp.sum(weights, axis=1, keepdims=True),
                    highest,
                    carry,
                )
            )
        own_parts.append(halves)
    acc[...] = jnp.zeros_like(acc)
    den[...] = jnp.zeros_like(den)

    def process(block):
        d = (block > me).astype(jnp.int32)
        for h in range(head_count):
            _, _, k_all, start, dk = queries[h]
            s = scores_of(h, k_all[block, :, start : start + dk])
            weights = s * col_weight[d, h, pl.ds(block, 1), :]
            vals = values_all[block, :, h * dv : (h + 1) * dv]
            acc[d, h] += weighted_values(weights, vals)
            den[d, h] += weights

    def arrive(kind, block, there, target):
        each(kv_copies(kind, block, False, pair), "wait_recv")

        @pl.when(there)
        def _():
            each(kv_copies(kind, block, False, target), "start")

        each(kv_copies(0, block, False, pair), "start")

    def from_pair(block):
        each(kv_copies(0, block, False, pair), "wait_recv")
        process(block)

    def step(d, carry):
        low_ok, high_ok = station - d >= 0, station + d < stations
        low, high = me - 2 * d, me + 2 * d

        @pl.when(low_ok)
        def _():
            arrive(1, low, up_there, me + 2)

        @pl.when(high_ok)
        def _():
            arrive(2, high, down_there, me - 2)

        @pl.when(low_ok)
        def _():
            process(low)

        @pl.when(high_ok)
        def _():
            process(high)

        @pl.when(station - (d - 1) >= 0)
        def _():
            from_pair(pair - 2 * (d - 1))

        @pl.when((station + (d - 1) < stations) & (d > 1))
        def _():
            from_pair(pair + 2 * (d - 1))

        return carry

    lax.fori_loop(1, stations, step, 0)
    last = stations - 1

    @pl.when(station - last >= 0)
    def _():
        from_pair(pair - 2 * last)

    if last > 0:

        @pl.when(station + last < stations)
        def _():
            from_pair(pair + 2 * last)

    merged_parts = []
    for h in range(head_count):
        total = None
        for d in range(2):
            own_num, own_den, highest, carry = own_parts[h][d]
            num = carry * acc[d, h] + own_num
            div = carry * jnp.sum(den[d, h], axis=1, keepdims=True) + own_den
            part = num / jnp.maximum(jnp.abs(div), jnp.exp(-highest))
            total = part if total is None else total + part
        total = total * lax.rsqrt(jnp.mean(total * total, axis=1, keepdims=True) + norm_eps)
        total = total * head_gain[:, h * dv : (h + 1) * dv]
        cut = slice(h * dv, (h + 1) * dv)
        merged = (residual[:, cut].astype(jnp.float32) + total).astype(jnp.bfloat16)
        merged_parts.append(merged)

    lane = lax.broadcasted_iota(jnp.int32, (rows, rows), 1)
    def column_of(row):
        return jnp.sum(jnp.where(t_iota == s_iota, row, 0), axis=1, keepdims=True)

    picks = [
        column_of(route_experts[p : p + 1, :].astype(jnp.float32)).astype(jnp.int32)
        for p in range(route_experts.shape[0])
    ]
    mixes = [column_of(route_weights[p : p + 1, :]) for p in range(route_experts.shape[0])]
    named = jnp.zeros((rows, rows), jnp.float32)
    for pick in picks:
        named = named + (lane == pick).astype(jnp.float32)
    named = named.astype(jnp.bfloat16)
    rank = jnp.dot(strict_low.astype(jnp.bfloat16), named, preferred_element_type=jnp.float32)
    over_rows = (((0,), (0,)), ((), ()))
    rank_t = lax.dot_general(
        named, strict_up.astype(jnp.bfloat16), over_rows, preferred_element_type=jnp.float32
    )
    named_t = lax.dot_general(
        named,
        (t_iota == s_iota).astype(jnp.bfloat16),
        over_rows,
        preferred_element_type=jnp.float32,
    )
    rank_t = jnp.where(named_t > 0.5, rank_t, -1.0)
    slot_iota = lax.broadcasted_iota(jnp.int32, (cap, rows), 0).astype(jnp.float32)

    merged = jnp.concatenate(merged_parts, axis=1)
    merged_f = merged.astype(jnp.float32)
    for e in range(n):
        choose = (slot_iota == rank_t[e : e + 1, :]).astype(jnp.bfloat16)
        slots_out[e] = jnp.dot(choose, merged, preferred_element_type=jnp.float32).astype(
            jnp.bfloat16
        )

    offsets = [(k + 1) // 2 if k % 2 else (n - k // 2) % n for k in range(n)]

    def back_of(k):
        return (me - offsets[k] + n) % n

    def ahead_of(k):
        return (me + offsets[k]) % n

    def row_copy(kind, k):
        if kind == 0:
            return remote(
                slots_out.at[ahead_of(k)],
                rows_in.at[col, me],
                row_send.at[0, k],
                row_recv.at[0, k],
                ahead_of(k),
                col,
            )
        source = back_of(k)
        column, target = ((col, cross), (col, sib), (cross, sib))[kind - 1]
        return remote(
            rows_in.at[column, source],
            rows_in.at[column, source],
            row_send.at[kind, k],
            row_recv.at[kind, k],
            me,
            target,
        )

    def row_arrival(kind, k):
        source = back_of(k)
        column = (col, cross, sib, cross_sib)[kind]
        return remote(
            rows_in.at[column, source],
            rows_in.at[column, source],
            row_send.at[kind, k],
            row_recv.at[kind, k],
            (me + k) % n,
            sib,
        )

    for k in range(1, n):
        row_copy(0, k).start()
    rows_in[col, me] = slots_out[me]

    def spread(ks):
        for k in ks:
            if k > 0:
                row_arrival(0, k).wait_recv()
            row_copy(1, k).start()
            row_copy(2, k).start()

    def relay(ks):
        for k in ks:
            row_arrival(1, k).wait_recv()
            row_copy(3, k).start()

    def members(g):
        return range(g * per_group, (g + 1) * per_group)

    def prepare(g):
        for k in members(g):
            row_arrival(2, k).wait_recv()
            row_arrival(3, k).wait_recv()
            at = (k - g * per_group) * cap
            parts = [rows_in[c, back_of(k)].astype(jnp.float32) for c in range(n_tp)]
            square = sum(jnp.sum(part * part, axis=1, keepdims=True) for part in parts)
            scale = lax.rsqrt(square / (width * n_tp) + norm_eps)
            for c, part in enumerate(parts):
                cut = slice(c * width, (c + 1) * width)
                lhs[at : at + cap, cut] = (part * scale * norm_gain[:, cut]).astype(jnp.bfloat16)

    def gate_up(g):
        if g == 0:
            for copy in fetch:
                copy.wait()
        features = lhs[...]
        gate_proj = jnp.dot(features, gate_w[...], preferred_element_type=jnp.float32)
        up_proj = jnp.dot(features, up_w[...], preferred_element_type=jnp.float32)
        hidden[...] = (gate_proj * jax.nn.sigmoid(gate_proj) * up_proj).astype(jnp.bfloat16)

    def down(g):
        for i, c in enumerate((cross_sib, cross, sib, col)):
            part = jnp.dot(
                hidden[...],
                down_w[:, pl.ds(pl.multiple_of(c * width, width), width)],
                preferred_element_type=jnp.float32,
            )
            partial_out[c, g] = part.astype(jnp.bfloat16)
            if i % 2 == 0:
                sib_copy(i // 2, g).start()

    def sib_copy(i, g):
        return remote(
            partial_out.at[(cross_sib, sib)[i], g],
            sib_in.at[i, g],
            sib_send.at[i, g],
            sib_recv.at[i, g],
            me,
            sib,
        )

    piece = group_rows // pieces

    def cross_copy(g, i):
        cut = slice(i * piece, (i + 1) * piece)
        return remote(
            pair_sum.at[g, cut],
            cross_in.at[g, cut],
            cross_send.at[g, i],
            cross_recv.at[g, i],
            me,
            cross,
        )

    def add_pair(g):
        sib_copy(0, g).wait_recv()
        for i in range(pieces):
            cut = slice(i * piece, (i + 1) * piece)
            pair_sum[g, cut] = (
                partial_out[cross, g, cut].astype(jnp.float32)
                + sib_in[0, g, cut].astype(jnp.float32)
            ).astype(jnp.bfloat16)
            cross_copy(g, i).start()

    def back_copy(k, arriving):
        g, at = k // per_group, (k % per_group) * cap
        expert_at = ahead_of(k) if arriving else me
        return remote(
            final.at[g, at : at + cap],
            back.at[expert_at],
            back_send.at[k],
            back_recv.at[k],
            back_of(k),
            col,
        )

    def finish(g):
        sib_copy(1, g).wait_recv()
        per_piece = per_group // pieces
        for i in range(pieces):
            cut = slice(i * piece, (i + 1) * piece)
            cross_copy(g, i).wait_recv()
            final[g, cut] = (
                partial_out[col, g, cut].astype(jnp.float32)
                + sib_in[1, g, cut].astype(jnp.float32)
                + cross_in[g, cut].astype(jnp.float32)
            ).astype(jnp.bfloat16)
            first = g * per_group + i * per_piece
            for k in range(first, first + per_piece):
                if k > 0:
                    back_copy(k, False).start()
        if g == 0:
            back[me] = final[0, 0:cap, :]

    late = members(1)
    half = per_group // 2
    spread(members(0))
    spread(late[:half])
    relay(members(0))
    prepare(0)
    gate_up(0)
    spread(late[half:])
    down(0)
    add_pair(0)
    relay(late)
    prepare(1)
    gate_up(1)
    down(1)
    add_pair(1)
    finish(0)
    finish(1)

    wide_lane = lax.broadcasted_iota(jnp.int32, (rows, n * cap), 1)
    takes = []
    for pick in picks:
        place = jnp.sum(jnp.where(lane == pick, rank, 0.0), axis=1, keepdims=True)
        slot = pick * cap + place.astype(jnp.int32)
        takes.append((wide_lane == slot).astype(jnp.bfloat16))
    for k in range(1, n):
        back_copy(k, True).wait_recv()
    returned = back[...].reshape(n * cap, width)
    added = merged_f
    for p, take in enumerate(takes):
        added = added + mixes[p] * jnp.dot(
            take, returned, preferred_element_type=jnp.float32
        )
    out_held[...] = added.astype(jnp.bfloat16)
    store = pltpu.make_async_copy(out_held, out, out_sem)
    store.start()

    for k in range(1, n):
        gate_copy(k, me).wait_send()
        row_copy(0, k).wait_send()
        back_copy(k, False).wait_send()
    for k in range(n):
        for kind in (1, 2, 3):
            row_copy(kind, k).wait_send()
    for g in range(groups):
        sib_copy(0, g).wait_send()
        sib_copy(1, g).wait_send()
        for i in range(pieces):
            cross_copy(g, i).wait_send()

    each(kv_copies(0, me, False, pair), "wait_send")

    @pl.when(up_there)
    def _():
        each(kv_copies(1, me, False, me + 2), "wait_send")

    @pl.when(down_there)
    def _():
        each(kv_copies(2, me, False, me - 2), "wait_send")

    def drain(d, carry):
        @pl.when(station - d >= 0)
        def _():
            each(kv_copies(0, me - 2 * d, False, pair), "wait_send")

            @pl.when(up_there)
            def _():
                each(kv_copies(1, me - 2 * d, False, me + 2), "wait_send")

        @pl.when(station + d < stations)
        def _():
            each(kv_copies(0, me + 2 * d, False, pair), "wait_send")

            @pl.when(down_there)
            def _():
                each(kv_copies(2, me + 2 * d, False, me - 2), "wait_send")

        return carry

    lax.fori_loop(1, stations, drain, 0)
    store.wait()


def layer(
    residual,
    query_wide,
    key_wide,
    query_narrow,
    key_narrow,
    values,
    gate_logits,
    head_gain,
    norm_gain,
    route_experts,
    route_weights,
    expert_gate,
    expert_up,
    expert_down,
    n,
    n_tp,
):
    rows, width = residual.shape
    head_count = gate_logits.shape[1]
    cap = 2 * route_experts.shape[1] * rows // n
    groups = 2
    pieces = 4
    group_rows = n // groups * cap
    dv = width // head_count
    bf, f32 = jnp.bfloat16, jnp.float32
    operands = (
        residual,
        query_wide,
        key_wide,
        query_narrow,
        key_narrow,
        values,
        gate_logits.reshape(4 * head_count, rows),
        head_gain.reshape(1, -1),
        norm_gain.reshape(1, -1),
        route_experts.T,
        route_weights.T,
        expert_gate,
        expert_up,
        expert_down,
    )
    hbm = pl.BlockSpec(memory_space=pl.ANY)
    dma = pltpu.SemaphoreType.DMA
    return pl.pallas_call(
        functools.partial(layer_kernel, n, groups, pieces, head_count // 2),
        out_shape=jax.ShapeDtypeStruct((rows, width), bf),
        in_specs=[hbm] * len(operands),
        out_specs=hbm,
        scratch_shapes=[pltpu.VMEM(a.shape, a.dtype) for a in operands[:-3]]
        + [
            pltpu.VMEM((n, 4 * head_count, rows), f32),
            pltpu.VMEM((n,) + key_wide.shape, bf),
            pltpu.VMEM((n,) + key_narrow.shape, bf),
            pltpu.VMEM((n,) + values.shape, bf),
            pltpu.VMEM((2, head_count, n, rows), f32),
            pltpu.VMEM((2, head_count, rows, dv), f32),
            pltpu.VMEM((2, head_count, rows, rows), f32),
            pltpu.VMEM((n, cap, width), bf),
            pltpu.VMEM((n_tp, n, cap, width), bf),
            pltpu.VMEM((group_rows, n_tp * width), bf),
            pltpu.VMEM((group_rows, expert_down.shape[1]), bf),
            pltpu.VMEM((n_tp, groups, group_rows, width), bf),
            pltpu.VMEM((2, groups, group_rows, width), bf),
            pltpu.VMEM((groups, group_rows, width), bf),
            pltpu.VMEM((groups, group_rows, width), bf),
            pltpu.VMEM((groups, group_rows, width), bf),
            pltpu.VMEM((n, cap, width), bf),
            pltpu.VMEM(expert_gate.shape[1:], bf),
            pltpu.VMEM(expert_up.shape[1:], bf),
            pltpu.VMEM(expert_down.shape[1:], bf),
            pltpu.VMEM((rows, width), bf),
            dma((3,)),
            dma((len(operands) - 3,)),
            dma,
            dma((n,)),
            dma((n,)),
            dma((3, 3, n)),
            dma((3, n)),
            dma((4, n)),
            dma((4, n)),
            dma((2, groups)),
            dma((2, groups)),
            dma((groups, pieces)),
            dma((groups, pieces)),
            dma((n,)),
            dma((n,)),
        ],
        compiler_params=pltpu.CompilerParams(
            collective_id=0, has_side_effects=True, vmem_limit_bytes=60 * 1024 * 1024
        ),
    )(*operands)


def fits(n, n_tp, args):
    rows = args[0].shape[0]
    cap = 2 * args[9].shape[1] * rows // n
    return n_tp == 4 and n % 8 == 0 and n <= 128 and rows == 128 and cap % 16 == 0


def choose(n, n_tp, *args):
    if fits(n, n_tp, args):
        return layer(*args, n, n_tp)
    return body(*args)


def solution(mesh):
    return jax.shard_map(
        functools.partial(choose, mesh.shape["sp"], mesh.shape["tp"]),
        mesh=mesh,
        in_specs=(
            P("sp", "tp"),
            P("sp", "tp"),
            P("sp", "tp"),
            P("sp", "tp"),
            P("sp", "tp"),
            P("sp", "tp"),
            P(None, "tp", "sp"),
            P("tp"),
            P(),
            P("sp", None),
            P("sp", None),
            P("sp", None, "tp"),
            P("sp", None, "tp"),
            P("sp", "tp", None),
        ),
        out_specs=P("sp", "tp"),
        check_vma=False,
    )
```
